256 devices in a mesh: ep: 32 (over z, x), tp: 8 (over y, core).
Axes of the slice: x: 4, y: 4, z: 8, core: 2. Of those that a mesh axis runs over, the one named last changes fastest.
Arguments:
- tokens: bfloat16 [16384, 4096], P('ep', 'tp'), may hold values from -60 to 60
- routes: int32 [16384, 4], P('ep'), may hold values from 0 to 127, all different within a row; in each aligned block of 512 rows (0 to 511, 512 to 1023, ...) at most 32 rows name the same one
- route_weights: float32 [16384, 4], P('ep'), may hold values from 0.1 to 1
- pre_gain: float32 [4096], P('tp'), may hold values from 0.1 to 1.9
- expert_gate: bfloat16 [128, 4096, 512], P('ep', 'tp'), may hold values from -0.09375 to 0.09375
- expert_up: bfloat16 [128, 4096, 512], P('ep', 'tp'), may hold values from -0.09375 to 0.09375
- expert_down: bfloat16 [128, 512, 4096], P('ep', None, 'tp'), may hold values from -1 to 1
- shared_gate: bfloat16 [4096, 512], P('tp'), may hold values from -0.09375 to 0.09375
- shared_up: bfloat16 [4096, 512], P('tp'), may hold values from -0.09375 to 0.09375
- shared_down: bfloat16 [512, 4096], P(None, 'tp'), may hold values from -1 to 1
- post_gain: float32 [4096], P('tp'), may hold values from 0.1 to 1.9
Outputs:
- layer_out: bfloat16 [16384, 4096], P('ep', 'tp')
The draws below stay inside these ranges and needn't reach their ends.
Inputs may be any that keep to these rules, and one draw needn't show every extreme that they name: `routes`: each row names 4 different experts. Within each aligned block of 512 rows (the tokens of one index of ep) no expert is named more than 32 times, a bound that some block reaches.
All inputs are finite; a program needn't handle non-finite values.
Results may differ from the reference program's by a relative error of at most 0.022.
Values may be sent and summed in bfloat16 or wider, within the bound.
No kernel may reach another device: no remote copies, remote signals or barrier semaphores. Data moves between devices by JAX's collectives and lax.ppermute only.
A program may use at most 128 MiB of HBM per device.

```python
import math
import jax
import jax.numpy as jnp
import numpy as np
from jax import lax

D = 4096
FF = 512
FS = 512
TOPK = 4
TOK_EP = 512
EXPERTS = 128
TOKENS = 16384
CAP = 32
N_EP = 32
N_TP = 8


def draw_tokens(key, part):
    key_base, key_rows, key_cols = jax.random.split(key, 3)
    ramp = 3.0 ** (jnp.arange(D, dtype=jnp.float32) / D)
    columns = ramp * jax.random.uniform(key_cols, (D,), jnp.float32, 0.5, 2.0)
    scales = jnp.exp(jax.random.uniform(key_rows, (TOKENS, 1), jnp.float32, -1.0, 1.0))
    base = jnp.clip(jax.random.normal(key_base, (TOKENS, D), jnp.float32), -6.0, 6.0)
    return jnp.clip(base * scales * columns, -60.0, 60.0).astype(jnp.bfloat16)


def ramped_weight(key, shape, fan_in):
    key_base, key_cols = jax.random.split(key)
    ramp = 3.0 ** (jnp.arange(D, dtype=jnp.float32) / D)
    columns = ramp * jax.random.uniform(key_cols, (D,), jnp.float32, 0.5, 2.0) / 2.0
    base = jnp.clip(jax.random.normal(key_base, shape, jnp.float32), -6.0, 6.0) * fan_in ** (-0.5)
    return jnp.clip(base * columns, -1.0, 1.0).astype(jnp.bfloat16)


def draw_expert_down(key, part):
    return ramped_weight(key, (EXPERTS, FF, D), FF)


def draw_shared_down(key, part):
    return ramped_weight(key, (FS, D), FS)


def steps_of(rng, dims, cuts, low, top_value):
    def one(position, shards_of):
        steps = jax.random.uniform(jax.random.fold_in(jax.random.fold_in(rng, 6), position), (shards_of,), jnp.float32, low / len(cuts), top_value / len(cuts))
        return jnp.repeat(jnp.exp(steps), dims[position] // shards_of).reshape((-1,) + (1,) * (len(dims) - position - 1))

    factor_of = one(*cuts[0])
    for cut in cuts[1:]:
        factor_of = factor_of * one(*cut)
    return factor_of


def routed_block(rng, own, number, rows, number_of, top, limit, slope):
    ranking = jax.random.permutation(rng, number_of)
    heavy_load, usual = shares(number_of, rows * top, limit, slope, True), shares(number_of, rows * top, limit, slope, False)
    places = jnp.arange(number_of)

    def named(sizes, offset_by):
        used = int((sizes > 0).sum())
        fixed = max(1, used // 4)
        moved = fixed + (places - fixed + offset_by * (used - fixed)) % max(1, number_of - fixed)
        return jnp.zeros((number_of,), jnp.int32).at[ranking[jnp.where(places < fixed, places, moved)]].set(jnp.asarray(sizes, jnp.int32))

    sizes = jnp.where(number % 4 == 0, named(heavy_load, number // 4), named(usual, number - number // 4 - 1))
    mixed = jax.random.permutation(jax.random.fold_in(own, 3), number_of)
    source_of, sink = mixed[0:number_of // 2 * 2:2], mixed[1:number_of // 2 * 2:2]
    slack = jnp.minimum(sizes[source_of] - 1, limit - sizes[sink]) // 2
    slack = jnp.where((source_of == ranking[0]) | (sink == ranking[0]) | (sizes[sink] == 0), 0, jnp.maximum(slack, 0))
    moved = jax.random.randint(jax.random.fold_in(own, 4), (number_of // 2,), 0, 1 << 20) % (slack + 1)
    sizes = sizes.at[source_of].add(-moved).at[sink].add(moved)
    labels = jnp.searchsorted(jnp.cumsum(sizes), jnp.arange(rows * top), side="right").astype(jnp.int32)
    table = labels.reshape(top, rows).T
    table = table[jax.random.permutation(jax.random.fold_in(own, 1), rows)]
    offset_by = jax.random.randint(jax.random.fold_in(own, 2), (rows, 1), 0, top)
    return jnp.take_along_axis(table, (jnp.arange(top)[None, :] + offset_by) % top, axis=1)


def shares(count, total, reach, lean, full):
    portions = [(1 << 20) // math.isqrt(grade ** lean) + 1 for grade in range(1, count + 1)]
    largest = reach if full else min(reach, max(-(-total // count), total * portions[0] // sum(portions)))
    least = 1 if total - largest >= count - 1 else 0
    counts, surplus = [largest] + [least] * (count - 1), total - largest - least * (count - 1)
    while surplus > 0:
        candidates = [i for i in range(1, count) if counts[i] < largest] or [i for i in range(1, count) if counts[i] < reach]
        mass, budget = sum([portions[i] for i in candidates]), surplus
        for i in candidates:
            extra = min(reach - counts[i], max(1, budget * portions[i] // mass), surplus)
            counts[i] = counts[i] + extra
            surplus = surplus - extra
    return np.array(counts)


def centred(rng, shape, width, reach, cuts=(), kind=jnp.bfloat16):
    gain = steps_of(rng, shape, cuts, -0.22, 0.18) if cuts else 1.0
    drawn = jax.random.normal(rng, shape, jnp.float32) * width * gain
    return jnp.minimum(jnp.maximum(drawn, -reach), reach).astype(kind)


def setup_inputs(seed: int = 0) -> dict:
    streams_of = jax.random.split(jax.random.key(seed), 12)
    tokens = draw_tokens(jax.random.fold_in(streams_of[11], 71), 0)
    routes_keys = jax.random.split(jax.random.fold_in(streams_of[1], 1), TOKENS // TOK_EP)
    routes_turns = jax.random.permutation(jax.random.fold_in(streams_of[1], 3), TOKENS // TOK_EP)
    routes = jax.vmap(lambda own, number: routed_block(jax.random.fold_in(streams_of[1], 2), own, number, TOK_EP, EXPERTS, TOPK, CAP, 2))(routes_keys, routes_turns).reshape((TOKENS, TOPK))
    route_weights = jnp.clip(jnp.exp(math.log(1.0) - 2.3025851 * jax.random.uniform(streams_of[2], (TOKENS, TOPK), jnp.float32) ** steps_of(streams_of[2], (TOKENS, TOPK), ((0, 32),), -0.2, 0.2)), 0.1, 1.0)
    pre_gain = jnp.clip(1.0 + 0.18 * jax.random.normal(streams_of[3], (D,), jnp.float32), 0.1, 1.9)
    expert_gate = centred(streams_of[4], (EXPERTS, D, FF), D ** -0.5, 0.09375, ((0, 32), (1, 8)))
    expert_up = centred(streams_of[5], (EXPERTS, D, FF), D ** -0.5, 0.09375, ((0, 32), (1, 8)))
    expert_down = draw_expert_down(jax.random.fold_in(streams_of[11], 71), 0)
    shared_gate = centred(streams_of[7], (D, FS), D ** -0.5, 0.09375, ((0, 8),))
    shared_up = centred(streams_of[8], (D, FS), D ** -0.5, 0.09375, ((0, 8),))
    shared_down = draw_shared_down(jax.random.fold_in(streams_of[11], 71), 0)
    post_gain = jnp.clip(1.0 + 0.18 * jax.random.normal(streams_of[10], (D,), jnp.float32), 0.1, 1.9)
    return {"tokens": tokens, "routes": routes, "route_weights": route_weights, "pre_gain": pre_gain, "expert_gate": expert_gate, "expert_up": expert_up, "expert_down": expert_down, "shared_gate": shared_gate, "shared_up": shared_up, "shared_down": shared_down, "post_gain": post_gain}


epsilon = 1e-06

def inverse_norm(values):
    return lax.rsqrt(lax.optimization_barrier(jnp.mean(values * values, axis=1)) + epsilon)

def blocked_product(inputs, weight):
    row_count = inputs.shape[0]
    out_width = weight.shape[1]
    pieces = inputs.reshape(row_count, N_TP, D // N_TP).astype(jnp.float32)
    blocks = weight.reshape(N_TP, D // N_TP, out_width).astype(jnp.float32)
    partial_value = jnp.einsum('rnd,ndf->nrf', pieces, blocks)
    rounded = lax.optimization_barrier(partial_value.astype(jnp.bfloat16))
    return lax.optimization_barrier(jnp.sum(rounded.astype(jnp.float32), axis=0))

def reference(tokens, routes, route_weights, pre_gain, expert_gate, expert_up, expert_down, shared_gate, shared_up, shared_down, post_gain):
    inputs = tokens.astype(jnp.float32)
    normed = (inputs * inverse_norm(inputs)[:, None] * pre_gain.astype(jnp.float32)).astype(jnp.bfloat16)
    per_block = TOK_EP * TOPK
    flat_ids = routes.reshape(N_EP, per_block).astype(jnp.int32)
    one_hot = (flat_ids[:, :, None] == jnp.arange(EXPERTS, dtype=jnp.int32)[None, None, :]).astype(jnp.int32)
    slots = lax.optimization_barrier(jnp.sum(jnp.cumsum(one_hot, axis=1) * one_hot, axis=2)) - 1
    sources = jnp.arange(N_EP, dtype=jnp.int32)[:, None]
    positions = (sources * CAP + slots).reshape(-1).astype(jnp.int32)
    token_index = (sources * TOK_EP + jnp.arange(per_block, dtype=jnp.int32)[None, :] // TOPK).reshape(-1).astype(jnp.int32)
    expert_index = flat_ids.reshape(-1)
    token_table = jnp.full((EXPERTS, N_EP * CAP), TOKENS, jnp.int32).at[expert_index, positions].set(token_index)
    weight_table = jnp.zeros((EXPERTS, N_EP * CAP), jnp.float32).at[expert_index, positions].set(route_weights.reshape(-1).astype(jnp.float32))

    def expert_step(totals, stacked):
        table_rows, table_weights, gate_weight, up_weight, down_weight = stacked
        arrived = jnp.take(normed, table_rows, axis=0, mode='fill', fill_value=0)
        gate_pre = blocked_product(arrived, gate_weight)
        up_pre = blocked_product(arrived, up_weight)
        hidden = (jax.nn.silu(gate_pre) * up_pre).astype(jnp.bfloat16)
        expert_out = jnp.dot(hidden, down_weight, preferred_element_type=jnp.float32).astype(jnp.bfloat16)
        totals = totals.at[table_rows].add(table_weights[:, None] * expert_out.astype(jnp.float32), mode='drop')
        return (totals, None)
    routed, _ = lax.scan(expert_step, jnp.zeros((TOKENS, D), jnp.float32), (token_table, weight_table, expert_gate, expert_up, expert_down))
    shared_gate_pre = blocked_product(normed, shared_gate)
    shared_up_pre = blocked_product(normed, shared_up)
    shared_hidden = (jax.nn.silu(shared_gate_pre) * shared_up_pre).astype(jnp.bfloat16)
    shared_out = jnp.dot(shared_hidden, shared_down, preferred_element_type=jnp.float32).astype(jnp.bfloat16)
    mixture = routed + shared_out.astype(jnp.float32)
    return (mixture * inverse_norm(mixture)[:, None] * post_gain.astype(jnp.float32)).astype(jnp.bfloat16)
```

```python
import jax
import jax.numpy as jnp
from jax import lax
from jax.experimental import pallas as pl
from jax.experimental.pallas import tpu as pltpu
from jax.sharding import Mesh, PartitionSpec as P


epsilon = 1e-06
f32 = jnp.float32
bf16 = jnp.bfloat16
i32 = jnp.int32

NZ, NX, NY, NC = 8, 4, 4, 2
T = 512
F = 512
SLOTS = 32
HALF = 16
EXTRA = 16


def shift(array, axis, by):
    n = lax.axis_size(axis)
    return lax.ppermute(array, axis, [(i, (i + by) % n) for i in range(n)])


def kernel_call(body, outs, ins, scratch=(), flops=0):
    n_bytes = sum(a.size * a.dtype.itemsize for a in ins) + sum(
        2 * o.size for o in outs
    )
    in_specs = [pl.BlockSpec(memory_space=pltpu.SMEM)] + [
        pl.BlockSpec(memory_space=pltpu.VMEM) for _ in ins[1:]
    ]
    return pl.pallas_call(
        body,
        out_shape=outs,
        in_specs=in_specs,
        out_specs=[pl.BlockSpec(memory_space=pltpu.VMEM) for _ in outs],
        scratch_shapes=list(scratch),
        cost_estimate=pl.CostEstimate(
            flops=flops, bytes_accessed=n_bytes, transcendentals=0
        ),
    )(*ins)


def dot(a, b):
    return jnp.dot(a, b, preferred_element_type=f32)


def row_ids(ids, extra):
    z, x, c = ids[0], ids[1], ids[3]
    route = extra[0:4].astype(i32)
    slot = extra[4:8].astype(i32)
    expert = route & 3
    valid = ((route >> 4) == z) & ((expert >> 1) == c)
    hop = ((route >> 2) - x) & 3
    portion = (expert & 1) * 2 + (slot >> 4)
    return jnp.where(valid, (hop * 4 + portion) * HALF + (slot & 15), -1)


def dispatch(ids, own, other):
    nb = len(own)
    rows = NX * 4 * HALF

    def body(ids_ref, *refs):
        own_refs, other_refs, outs = refs[:nb], refs[nb : 2 * nb], refs[2 * nb :]
        row = lax.broadcasted_iota(i32, (rows, T), 0)
        for b in range(nb):
            extra = own_refs[b][T : T + EXTRA, :].astype(f32)
            ids = row_ids(ids_ref, extra)
            hit = row == ids[0:1]
            for k in range(1, 4):
                hit = hit | (row == ids[k : k + 1])
            pick = jnp.where(hit, 1.0, 0.0).astype(bf16)
            for at, ref in ((0, own_refs[b]), (F, other_refs[b])):
                picked = dot(pick, ref[0:T, :]).astype(bf16)
                for s in range(NX):
                    outs[s][:, b * HALF : (b + 1) * HALF, at : at + F] = picked[
                        s * 64 : (s + 1) * 64
                    ].reshape(4, HALF, F)

    outs = [jax.ShapeDtypeStruct((4, nb * HALF, 2 * F), bf16)] * NX
    return kernel_call(
        body, outs, [ids, *own, *other], flops=2 * nb * rows * T * 2 * F
    )


def gate_up(ids, rows, weights, shared=None):
    nr = rows[0].shape[1]
    width = weights[0].shape[2]
    extra = 0 if shared is None else 64
    r = NX * nr

    def body(ids_ref, *refs):
        xs, ws = refs[:4], refs[4:8]
        refs = refs[8:]
        sh = refs[: 6 if extra else 0]
        refs = refs[len(sh) :]
        outs, held = refs[:4], refs[4]
        y, c = ids_ref[2], ids_ref[3]
        for j in range(2):
            stacked = jnp.concatenate(
                [xs[s][2 * j + h] for h in range(2) for s in range(NX)], axis=0
            )
            for at, mine, theirs in ((0, ws[0], ws[2]), (width, ws[1], ws[3])):
                part = dot(stacked[:, :F], mine[j]) + dot(stacked[:, F:], theirs[j])
                part = part.astype(bf16)
                for h in range(2):
                    held[2 * j + h, 0:r, at : at + width] = part[h * r : (h + 1) * r]
        if extra:
            mine = sh[0][pl.ds(pl.multiple_of(c * 256, 256), 256), :]
            theirs = sh[1][pl.ds(pl.multiple_of(c * 256, 256), 256), :]
            for at, own_w, other_w in ((0, sh[2], sh[4]), (width, sh[3], sh[5])):
                part = dot(mine, own_w[...]) + dot(theirs, other_w[...])
                held[:, r : r + extra, at : at + width] = part.astype(bf16).reshape(
                    4, extra, width
                )
        for t in range(NY):
            outs[t][...] = held[(y + t) & 3]

    outs = [jax.ShapeDtypeStruct((r + extra, 2 * width), bf16)] * NY
    ins = [ids, *rows, *weights] + ([] if shared is None else list(shared))
    return kernel_call(
        body,
        outs,
        ins,
        scratch=[pltpu.VMEM((4, r + extra, 2 * width), bf16)],
        flops=2 * 4 * (r + extra) * 2 * F * 2 * width,
    )


def down(ids, hidden, weights, nr, shared=None):
    width = hidden[0].shape[1]
    extra = 0 if shared is None else 64
    r = NX * nr

    def body(ids_ref, *refs):
        hs, ws = refs[:4], refs[4:6]
        refs = refs[6:]
        sh = refs[: 2 if extra else 0]
        refs = refs[len(sh) :]
        outs, refs = refs[:4], refs[4:]
        sh_outs = refs[: 2 if extra else 0]
        held = refs[-1]
        y = ids_ref[2]
        for t in range(NY):
            held[(y - t) & 3] = hs[t][...]
        for j in range(2):
            stacked = jnp.concatenate([held[2 * j + h, 0:r] for h in range(2)], axis=0)
            for at, w in ((0, ws[0]), (F, ws[1])):
                part = dot(stacked, w[j]).astype(bf16)
                for h in range(2):
                    for s in range(NX):
                        outs[s][2 * j + h, :, at : at + F] = part[
                            h * r + s * nr : h * r + (s + 1) * nr
                        ]
        if extra:
            stacked = held[:, r : r + extra, :].reshape(4 * extra, width)
            for out, w in zip(sh_outs, sh):
                out[...] = dot(stacked, w[...]).astype(bf16)

    outs = [jax.ShapeDtypeStruct((4, nr, 2 * F), bf16)] * NX
    ins = [ids, *hidden, *weights]
    if shared is not None:
        outs = outs + [jax.ShapeDtypeStruct((256, F), bf16)] * 2
        ins = ins + list(shared)
    return kernel_call(
        body,
        outs,
        ins,
        scratch=[pltpu.VMEM((4, r + extra, width), bf16)],
        flops=2 * 4 * (r + extra) * width * 2 * F,
    )


def combine(ids, extras, rows):
    nb = len(extras)
    width = NX * 4 * HALF

    def body(ids_ref, *refs):
        ex, ys, outs = refs[:nb], refs[nb : nb + 4], refs[nb + 4 :]
        lane = lax.broadcasted_iota(i32, (T, width), 1).astype(f32)
        for b in range(nb):
            extra = ex[b][...].astype(f32)
            table = jnp.concatenate(
                [row_ids(ids_ref, extra).astype(f32), extra[8:12]], axis=0
            ).T
            mix = jnp.zeros((T, width), f32)
            for k in range(4):
                mix = jnp.where(
                    lane == table[:, k : k + 1], table[:, 4 + k : 5 + k], mix
                )
            mix = mix.astype(bf16)
            stacked = jnp.concatenate(
                [
                    ys[s][:, b * HALF : (b + 1) * HALF, :].reshape(64, 2 * F)
                    for s in range(NX)
                ],
                axis=0,
            )
            outs[2 * b][...] = dot(mix, stacked[:, :F]).astype(bf16)
            outs[2 * b + 1][...] = dot(mix, stacked[:, F:]).astype(bf16)

    outs = [jax.ShapeDtypeStruct((T, F), bf16)] * (2 * nb)
    return kernel_call(
        body, outs, [ids, *extras, *rows], flops=2 * nb * T * width * 2 * F
    )


def tp_sum(values):
    chip = values + shift(values, "c", 1)
    return chip + shift(chip, "y", 1) + shift(chip, "y", 2) + shift(chip, "y", 3)


def inverse_norm(values):
    squares = jnp.sum(values * values, axis=1).reshape(4, 128)
    totals = tp_sum(squares).reshape(-1)
    return lax.rsqrt(totals / (F * NY * NC) + epsilon)


def slots_of(routes):
    experts = jnp.arange(128, dtype=i32)
    named = routes[:, :, None] == experts
    counts = jnp.sum(named.astype(f32), axis=1).astype(bf16)
    at = jnp.arange(T, dtype=i32)
    before = (at[None, :] < at[:, None]).astype(bf16)
    rank = dot(before, counts)
    return jnp.sum(jnp.where(named, rank[:, None, :], 0.0), axis=2)


def per_device(
    tokens,
    routes,
    route_weights,
    pre_gain,
    expert_gate,
    expert_up,
    expert_down,
    shared_gate,
    shared_up,
    shared_down,
    post_gain,
):
    z, x, y, c = (lax.axis_index(a) for a in ("z", "x", "y", "c"))
    ids = jnp.stack([z, x, y, c]).astype(i32)
    inputs = tokens.astype(f32)
    normed = (inputs * inverse_norm(inputs)[:, None] * pre_gain).astype(bf16)
    extra = jnp.concatenate(
        [routes.astype(f32), slots_of(routes), route_weights, jnp.zeros((T, 4), f32)],
        axis=1,
    )
    payload = jnp.concatenate([normed, extra.T.astype(bf16)], axis=0)

    block = {0: payload}
    for k in range(1, 4):
        block[-k] = shift(block[1 - k], "z", 1)
        block[k] = shift(block[k - 1], "z", -1)
    cut = 272
    block[4] = jnp.concatenate(
        [shift(block[-3][:cut], "z", 1), shift(block[3][cut:], "z", -1)], axis=0
    )

    def experts_of(weight):
        mine = lax.dynamic_slice_in_dim(weight, 2 * c, 2, axis=0)
        theirs = lax.dynamic_slice_in_dim(weight, 2 * (1 - c), 2, axis=0)
        return mine, shift(theirs, "c", 1)

    gate, gate_other = experts_of(expert_gate)
    up, up_other = experts_of(expert_up)
    down_own, down_other = experts_of(expert_down)
    s_gate, s_up, s_down = (shift(w, "c", 1) for w in (shared_gate, shared_up, shared_down))

    part_own, part_other = {}, {}
    for chunk in ((0, -1, 1), (-2, 2), (-3, 3), (4,)):
        first = chunk[0] == 0
        other = [shift(block[d], "c", 1) for d in chunk]
        sent = dispatch(ids, [block[d] for d in chunk], other)
        rows = [sent[0]] + [shift(sent[s], "x", s) for s in range(1, NX)]
        shared = (block[0], other[0], shared_gate, shared_up, s_gate, s_up) if first else None
        parts = gate_up(ids, rows, (gate, up, gate_other, up_other), shared)
        total = parts[0].astype(f32)
        for t in range(1, NY):
            total = total + shift(parts[t], "y", t).astype(f32)
        width = gate.shape[2]
        hidden = (jax.nn.silu(total[:, :width]) * total[:, width:]).astype(bf16)
        hidden = [hidden] + [shift(hidden, "y", t) for t in range(1, NY)]
        shared = (shared_down, s_down) if first else None
        outs = down(ids, hidden, (down_own, down_other), len(chunk) * HALF, shared)
        if first:
            shared_own, shared_other = outs[4], shift(outs[5], "c", 1)
        back = [outs[0]] + [shift(outs[s], "x", -s) for s in range(1, NX)]
        mixed = combine(ids, [block[d][T:] for d in chunk], back)
        for b, d in enumerate(chunk):
            part_own[d] = mixed[2 * b]
            part_other[d] = shift(mixed[2 * b + 1], "c", 1)

    def part(d):
        return part_own[d].astype(f32) + part_other[d].astype(f32)

    far = part(4).astype(bf16)
    half = T // 2
    rise = shift(far[:half], "z", 1).astype(f32)
    fall = shift(far[half:], "z", -1).astype(f32)
    near_up, near_down = part(3), part(-3)
    rise = jnp.concatenate([near_up[:half] + rise, near_up[half:]], axis=0)
    fall = jnp.concatenate([near_down[:half], near_down[half:] + fall], axis=0)
    for k in (2, 1, 0):
        rise = shift(rise.astype(bf16), "z", 1).astype(f32)
        fall = shift(fall.astype(bf16), "z", -1).astype(f32)
        if k:
            rise, fall = rise + part(k), fall + part(-k)
    shared_out = jnp.where(
        c == 0,
        jnp.concatenate([shared_own, shared_other], axis=0),
        jnp.concatenate([shared_other, shared_own], axis=0),
    )
    mixture = rise + fall + part(0) + shared_out.astype(f32)
    return (mixture * inverse_norm(mixture)[:, None] * post_gain).astype(bf16)


def solution(mesh):
    fine = Mesh(mesh.devices.reshape(NZ, NX, NY, NC), ("z", "x", "y", "c"))
    ep, tp = ("z", "x"), ("y", "c")
    in_specs = (
        P(ep, tp),
        P(ep, None),
        P(ep, None),
        P(tp),
        P(ep, tp, None),
        P(ep, tp, None),
        P(ep, None, tp),
        P(tp, None),
        P(tp, None),
        P(None, tp),
        P(tp),
    )
    return jax.shard_map(
        per_device, mesh=fine, in_specs=in_specs, out_specs=P(ep, tp), check_vma=False
    )
```
